32 devices in a mesh: grp: 2 (over y), sp: 4 (over z), tp: 4 (over x, core).
Axes of the slice: x: 2, y: 2, z: 4, core: 2. Of those that a mesh axis runs over, the one named last changes fastest.
Arguments:
- query_a: bfloat16 [2048, 2048], P(('grp', 'sp'), 'tp'), parts along dimension 0, may hold values from -6 to 6
- key_a: bfloat16 [2048, 2048], P(('grp', 'sp'), 'tp'), parts along dimension 0, may hold values from -6 to 6
- value_a: bfloat16 [2048, 4096], P(('grp', 'sp'), 'tp'), parts along dimension 0, may hold values from -6 to 6
- decay_a: float32 [2, 8, 2048], P(None, 'tp', ('grp', 'sp')), parts along dimension 2, may hold values from -1 to 0
- query_b: bfloat16 [2048, 1024], P(('grp', 'sp'), 'tp'), parts along dimension 0, may hold values from -6 to 6
- key_b: bfloat16 [2048, 1024], P(('grp', 'sp'), 'tp'), parts along dimension 0, may hold values from -6 to 6
- value_b: bfloat16 [2048, 1024], P(('grp', 'sp'), 'tp'), parts along dimension 0, may hold values from -6 to 6
- decay_b: float32 [2, 16, 2048], P(None, 'tp', ('grp', 'sp')), parts along dimension 2, may hold values from -1 to 0
- out_weight_a: bfloat16 [4096, 2048], P('tp'), may hold values from -0.078125 to 0.078125
- out_weight_b: bfloat16 [1024, 2048], P('tp'), may hold values from -0.078125 to 0.078125
- residual: bfloat16 [2048, 2048], P(('grp', 'sp', 'tp')), parts along dimension 0, may hold values from -6 to 6
- norm_gain: float32 [2, 2048], replicated, may hold values from 0.1 to 1.9
- route_group: int32 [2048], P(('grp', 'sp', 'tp')), parts along dimension 0, may hold values from 0 to 3
- route_expert: int32 [2048, 2], P(('grp', 'sp', 'tp')), parts along dimension 0, may hold values from 0 to 7, as said below
- route_weight: float32 [2048, 2], P(('grp', 'sp', 'tp')), parts along dimension 0, may hold values from 0.2 to 1
- expert_gate: bfloat16 [32, 2048, 1024], P('sp', None, 'tp'), may hold values from -0.125 to 0.125
- expert_up: bfloat16 [32, 2048, 1024], P('sp', None, 'tp'), may hold values from -0.125 to 0.125
- expert_down: bfloat16 [32, 1024, 2048], P('sp', 'tp'), may hold values from -0.1875 to 0.1875
Outputs:
- layer_out: bfloat16 [2048, 2048], P(('grp', 'sp', 'tp')), parts along dimension 0
The draws below stay inside these ranges and needn't reach their ends.
There are 2 independent parts, one for each index of `grp`. The reference program is written for one: setup_inputs(seed, part) draws one part's arguments, and reference() takes and returns one part's arrays. A program takes and returns all parts, laid end to end along the dimension named above; an argument that names none is the same for every part. Nothing has to cross between parts.
Inputs may be any that keep to these rules, and one draw needn't show every extreme that they name: `route_expert`: the 2 entries of a row are different.
All inputs are finite; a program needn't handle non-finite values.
Results may differ from the reference program's by a relative error of at most 0.015.
Values may be sent and summed in bfloat16 or wider, within the bound.
A program may use at most 128 MiB of HBM per device.

```python
import math
import jax
import jax.numpy as jnp
from jax import lax

D = 2048
HA = 8
DKA = 256
DVA = 512
HB = 16
DKB = 64
DVB = 64
BLOCK = 128
EXPERTS = 32
GROUPS = 4
FF = 1024
TOP = 2
CAP = 2
TOK_DEV = 256
TOKENS = 1024
ROWS_DEV = 64
EXP_GROUP = 8
N_TP = 4


def decay_law(key, number_of_heads):
    sequence_length = TOKENS
    key_rows = jax.random.split(key, 6)
    fast = jax.random.randint(key_rows[0], (2, number_of_heads), 0, 2) == 0
    fast_rate = jnp.exp(jax.random.uniform(key_rows[1], (2, number_of_heads), jnp.float32, jnp.log(0.01), jnp.log(1.0 / 30.0)))
    slow_rate = jnp.exp(jax.random.uniform(key_rows[2], (2, number_of_heads), jnp.float32, jnp.log(0.1), jnp.log(0.4))) / sequence_length
    rate = jnp.where(fast, fast_rate, slow_rate)
    devices = sequence_length // TOK_DEV
    factor = jnp.exp(jax.random.uniform(key_rows[3], (2, number_of_heads, devices), jnp.float32, -jnp.log(2.0), jnp.log(2.0)))
    factor = jnp.repeat(factor, TOK_DEV, axis=2)
    smoothing_factor = -rate[..., None] * factor
    spike_location = jax.random.randint(key_rows[4], (2, number_of_heads, 2), 0, sequence_length)
    spike_penalty = jnp.log(jax.random.uniform(key_rows[5], (2, number_of_heads, 2), jnp.float32, 0.5, 0.8))
    token_positions = jnp.arange(sequence_length, dtype=jnp.int32)
    spike_events = jnp.sum(jnp.where(token_positions[None, None, None, :] == spike_location[..., None], spike_penalty[..., None], 0.0), axis=2)
    return (smoothing_factor + spike_events).astype(jnp.float32)


def draw_decay_a(key, part):
    return decay_law(jax.random.fold_in(key, 11), HA)


def draw_decay_b(key, part):
    return decay_law(jax.random.fold_in(key, 12), HB)


def route_law(key):
    key_rows = jax.random.split(jax.random.fold_in(key, 7), 6)
    blocks = TOKENS // ROWS_DEV
    favored = jax.random.randint(key_rows[0], (), 0, EXPERTS)
    favored_group = favored // EXP_GROUP
    favored_slot = favored % EXP_GROUP
    group_draw = jax.random.randint(key_rows[1], (TOKENS,), 0, 2 * GROUPS)
    group_ids = jnp.where(group_draw >= GROUPS, favored_group, group_draw)
    first_pick = jax.random.randint(key_rows[2], (TOKENS,), 0, EXP_GROUP)
    leaning = (jax.random.randint(key_rows[3], (TOKENS,), 0, 3) == 0) & (group_ids == favored_group)
    first_pick = jnp.where(leaning, favored_slot, first_pick)
    scores = jax.random.randint(key_rows[4], (blocks, ROWS_DEV), 0, 1 << 20) * ROWS_DEV + jnp.arange(ROWS_DEV, dtype=jnp.int32)[None, :]
    ranking = jnp.argsort(jnp.argsort(scores, axis=1), axis=1)
    forced = (ranking < CAP).reshape(TOKENS)
    group_ids = jnp.where(forced, favored_group, group_ids)
    first_pick = jnp.where(forced, favored_slot, first_pick)
    second_pick = (first_pick + 1 + jax.random.randint(key_rows[5], (TOKENS,), 0, EXP_GROUP - 1)) % EXP_GROUP
    return (group_ids.astype(jnp.int32), jnp.stack([first_pick, second_pick], axis=1).astype(jnp.int32))


def draw_route_group(key, part):
    return route_law(key)[0]


def draw_route_expert(key, part):
    return route_law(key)[1]


def levels(own_key, extent, shards, least, largest):
    level = 1.0
    for dim, blocks in shards:
        steps = jax.random.uniform(jax.random.fold_in(jax.random.fold_in(own_key, 6), dim), (blocks,), jnp.float32, least / len(shards), largest / len(shards))
        level = level * jnp.repeat(jnp.exp(steps), extent[dim] // blocks).reshape((-1,) + (1,) * (len(extent) - 1 - dim))
    return level


def noise(key, extent, deviation, bound, cuts=(), held_as=jnp.bfloat16):
    values = deviation * jax.random.normal(key, extent, jnp.float32)
    if cuts:
        values = values * levels(key, extent, cuts, -0.22, 0.18)
    return jnp.clip(values, -bound, bound).astype(held_as)


def setup_inputs(seed: int = 0, part: int = 0) -> dict:
    splits = jax.random.split(jax.random.key(seed), 19)
    part_keys = jax.random.split(jax.random.fold_in(splits[18], part), 19)
    query_a = noise(part_keys[0], (TOKENS, HA * DKA), 1.0, 6.0, ((0, 4), (1, 4)))
    key_a = noise(part_keys[1], (TOKENS, HA * DKA), 1.0, 6.0, ((0, 4), (1, 4)))
    value_a = noise(part_keys[2], (TOKENS, HA * DVA), 1.0, 6.0, ((0, 4), (1, 4)))
    decay_a = draw_decay_a(jax.random.fold_in(jax.random.fold_in(splits[18], part), 71), part)
    query_b = noise(part_keys[4], (TOKENS, HB * DKB), 1.0, 6.0, ((0, 4), (1, 4)))
    key_b = noise(part_keys[5], (TOKENS, HB * DKB), 1.0, 6.0, ((0, 4), (1, 4)))
    value_b = noise(part_keys[6], (TOKENS, HB * DVB), 1.0, 6.0, ((0, 4), (1, 4)))
    decay_b = draw_decay_b(jax.random.fold_in(jax.random.fold_in(splits[18], part), 71), part)
    out_weight_a = noise(splits[8], (HA * DVA, D), (HA * DVA + HB * DVB) ** -0.5, 0.078125, ((0, 4),))
    out_weight_b = noise(splits[9], (HB * DVB, D), (HA * DVA + HB * DVB) ** -0.5, 0.078125, ((0, 4),))
    residual = noise(part_keys[10], (TOKENS, D), 1.0, 6.0, ((0, 16),))
    norm_gain = jnp.clip(1.0 + 0.18 * jax.random.normal(splits[11], (2, D), jnp.float32), 0.1, 1.9)
    route_group = draw_route_group(jax.random.fold_in(jax.random.fold_in(splits[18], part), 71), part)
    route_expert = draw_route_expert(jax.random.fold_in(jax.random.fold_in(splits[18], part), 71), part)
    route_weight = jnp.clip(0.2 + 0.8 * jax.random.uniform(part_keys[14], (TOKENS, TOP), jnp.float32) ** levels(part_keys[14], (TOKENS, TOP), ((0, 16),), -0.2, 0.2), 0.2, 1.0)
    expert_gate = noise(splits[15], (EXPERTS, D, FF), D ** -0.5, 0.125, ((0, 4), (2, 4)))
    expert_up = noise(splits[16], (EXPERTS, D, FF), D ** -0.5, 0.125, ((0, 4), (2, 4)))
    expert_down = noise(splits[17], (EXPERTS, FF, D), FF ** -0.5, 0.1875, ((0, 4), (1, 4)))
    return {"query_a": query_a, "key_a": key_a, "value_a": value_a, "decay_a": decay_a, "query_b": query_b, "key_b": key_b, "value_b": value_b, "decay_b": decay_b, "out_weight_a": out_weight_a, "out_weight_b": out_weight_b, "residual": residual, "norm_gain": norm_gain, "route_group": route_group, "route_expert": route_expert, "route_weight": route_weight, "expert_gate": expert_gate, "expert_up": expert_up, "expert_down": expert_down}


HIGHEST = lax.Precision.HIGHEST
RESIDUAL_SCALE = math.sqrt(2.0)
NORM_EPS = 1e-05
GROUP_EPS = 1e-06
ROPE_BASE = 10000.0

def rotate(vectors, token_positions):
    half_width = vectors.shape[-1] // 2
    frequencies = ROPE_BASE ** (-jnp.arange(half_width, dtype=jnp.float32) / half_width)
    angles = token_positions.astype(jnp.float32)[:, None] * frequencies[None, :]
    cosine = jnp.cos(angles)[:, None, :]
    sine_part = jnp.sin(angles)[:, None, :]
    first_half = vectors[..., :half_width].astype(jnp.float32)
    second = vectors[..., half_width:].astype(jnp.float32)
    return jnp.concatenate([first_half * cosine - second * sine_part, first_half * sine_part + second * cosine], axis=-1)

def sweep_blocks(queries, keys_rot, values, log_decay, strict, state_init, span_size):
    length, number_of_heads, key_dim = queries.shape
    value_dim = values.shape[-1]
    block_count = length // span_size

    def split_blocks(array):
        return array.reshape(block_count, span_size, number_of_heads, array.shape[-1])
    decay_blocks = log_decay.reshape(number_of_heads, block_count, span_size).transpose(1, 0, 2)
    position_index = jnp.arange(span_size)
    if strict:
        allowed = position_index[:, None] > position_index[None, :]
    else:
        allowed = position_index[:, None] >= position_index[None, :]

    def advance(state_now, inputs):
        query_blk, key_blk, value_blk, decay_blk = inputs
        cumulative = jnp.cumsum(decay_blk, axis=1)
        log_gap = cumulative[:, :, None] - cumulative[:, None, :]
        weights = jnp.where(allowed[None], jnp.exp(jnp.where(allowed[None], log_gap, 0.0)), 0.0)
        scores = jnp.einsum('ihd,jhd->hij', query_blk, key_blk, preferred_element_type=jnp.float32) * weights
        weighted = scores.astype(jnp.bfloat16)
        inner_part = jnp.einsum('hij,jhv->ihv', weighted, value_blk, preferred_element_type=jnp.float32)
        carried = jnp.einsum('ihd,hdv->ihv', query_blk.astype(jnp.float32), state_now, precision=HIGHEST) * jnp.exp(cumulative).T[:, :, None]
        key_scaled = key_blk.astype(jnp.float32) * jnp.exp(cumulative[:, -1:] - cumulative).T[:, :, None]
        state_next = state_now * jnp.exp(cumulative[:, -1])[:, None, None] + jnp.einsum('jhd,jhv->hdv', key_scaled, value_blk.astype(jnp.float32), precision=HIGHEST)
        return (state_next, inner_part + carried)
    final_state, outputs = lax.scan(advance, state_init, (split_blocks(queries), split_blocks(keys_rot), split_blocks(values), decay_blocks))
    return (outputs.reshape(length, number_of_heads, value_dim), final_state)

def retain(query_w, key_w, value_w, decay, number_of_heads):
    sequence_length = query_w.shape[0]
    token_positions = jnp.arange(sequence_length, dtype=jnp.int32)
    queries_f = rotate(query_w.reshape(sequence_length, number_of_heads, -1), token_positions)
    key_dim = queries_f.shape[-1]
    queries = queries_f.astype(jnp.bfloat16)
    keys_rot = (rotate(key_w.reshape(sequence_length, number_of_heads, -1), token_positions) * (1.0 / math.sqrt(key_dim))).astype(jnp.bfloat16)
    values = value_w.reshape(sequence_length, number_of_heads, -1)
    zero_state = jnp.zeros((number_of_heads, key_dim, values.shape[-1]), jnp.float32)
    forward = sweep_blocks(queries, keys_rot, values, decay[0], False, zero_state, BLOCK)[0]
    backward = sweep_blocks(queries[::-1], keys_rot[::-1], values[::-1], decay[1][:, ::-1], True, zero_state, BLOCK)[0]
    total_sum = forward + backward[::-1]
    normed = total_sum * lax.rsqrt(lax.optimization_barrier(jnp.mean(total_sum * total_sum, axis=-1, keepdims=True)) + GROUP_EPS)
    return normed.reshape(sequence_length, -1).astype(jnp.bfloat16)

def layer_norm(stream, gain):
    center = stream - lax.optimization_barrier(jnp.mean(stream, axis=-1, keepdims=True))
    spread = lax.optimization_barrier(jnp.mean(center * center, axis=-1, keepdims=True))
    return center * lax.rsqrt(spread + NORM_EPS) * gain

def slot_table(expert_ids):
    onehot = (expert_ids[..., None] == jnp.arange(EXPERTS, dtype=jnp.int32)).astype(jnp.int32)
    earlier = jnp.cumsum(onehot, axis=-2) - onehot
    rank_order = lax.optimization_barrier(jnp.sum(earlier * onehot, axis=-1))
    kept_mask = rank_order < CAP
    slot_index = expert_ids * CAP + jnp.minimum(rank_order, CAP - 1)
    return (slot_index.astype(jnp.int32), kept_mask)

def reference(query_a, key_a, value_a, decay_a, query_b, key_b, value_b, decay_b, out_weight_a, out_weight_b, residual, norm_gain, route_group, route_expert, route_weight, expert_gate, expert_up, expert_down):
    sequence_length = query_a.shape[0]
    mixed_a = retain(query_a, key_a, value_a, decay_a, HA)
    mixed_b = retain(query_b, key_b, value_b, decay_b, HB)
    shard_a = mixed_a.reshape(sequence_length, N_TP, -1).transpose(1, 0, 2)
    shard_b = mixed_b.reshape(sequence_length, N_TP, -1).transpose(1, 0, 2)
    weight_a = out_weight_a.reshape(N_TP, -1, D)
    weight_b = out_weight_b.reshape(N_TP, -1, D)

    def add_partial(total_sum, pieces):
        partial_value = jnp.dot(pieces[0], pieces[1], preferred_element_type=jnp.float32) + jnp.dot(pieces[2], pieces[3], preferred_element_type=jnp.float32)
        rounded = lax.optimization_barrier(partial_value.astype(jnp.bfloat16))
        return (total_sum + rounded.astype(jnp.float32), None)
    mix = lax.scan(add_partial, jnp.zeros((sequence_length, D), jnp.float32), (shard_a, weight_a, shard_b, weight_b))[0]
    hidden_in = layer_norm(RESIDUAL_SCALE * residual.astype(jnp.float32) + mix, norm_gain[0]).astype(jnp.bfloat16)
    blocks = sequence_length // ROWS_DEV
    slots = EXPERTS * CAP
    global_ids = route_group[:, None] * EXP_GROUP + route_expert
    slot_index, kept_mask = slot_table(global_ids.reshape(blocks, ROWS_DEV * TOP).astype(jnp.int32))
    hits = (slot_index[..., None] == jnp.arange(slots, dtype=jnp.int32)) & kept_mask[..., None]
    choose = lax.optimization_barrier(jnp.sum(hits.reshape(blocks, ROWS_DEV, TOP, slots).astype(jnp.float32), axis=2))
    outgoing = jnp.einsum('brs,brd->bsd', choose, hidden_in.reshape(blocks, ROWS_DEV, D).astype(jnp.float32))
    outgoing = outgoing.astype(jnp.bfloat16).reshape(blocks, EXPERTS, CAP, D).transpose(1, 0, 2, 3).reshape(EXPERTS, blocks * CAP, D)

    def expert_apply(inputs):
        rows, gate_w, up_w, down_w = inputs
        gate_part = jnp.dot(rows, gate_w, preferred_element_type=jnp.float32)
        up_part = jnp.dot(rows, up_w, preferred_element_type=jnp.float32)
        expert_hidden = (jax.nn.silu(gate_part) * up_part).astype(jnp.bfloat16)
        hidden_sets = expert_hidden.reshape(rows.shape[0], N_TP, -1).transpose(1, 0, 2)
        down_sets = down_w.reshape(N_TP, -1, D)

        def add_set(total_sum, pieces):
            partial_value = jnp.dot(pieces[0], pieces[1], preferred_element_type=jnp.float32)
            rounded = lax.optimization_barrier(partial_value.astype(jnp.bfloat16))
            return (total_sum + rounded.astype(jnp.float32), None)
        expert_sum = lax.scan(add_set, jnp.zeros((rows.shape[0], D), jnp.float32), (hidden_sets, down_sets))[0]
        return expert_sum.astype(jnp.bfloat16)
    expert_out = lax.map(expert_apply, (outgoing, expert_gate, expert_up, expert_down))
    returned = expert_out.reshape(EXPERTS, blocks, CAP, D).transpose(1, 0, 2, 3).reshape(blocks, slots, D)
    picked = jnp.take_along_axis(returned, slot_index[..., None], axis=1).astype(jnp.float32)
    picked = picked.reshape(blocks, ROWS_DEV, TOP, D)
    factor = jnp.where(kept_mask.reshape(blocks, ROWS_DEV, TOP), route_weight.reshape(blocks, ROWS_DEV, TOP), 0.0)
    ffn = lax.optimization_barrier(jnp.sum(picked * factor[..., None], axis=2)).reshape(sequence_length, D)
    return layer_norm(RESIDUAL_SCALE * hidden_in.astype(jnp.float32) + ffn, norm_gain[1]).astype(jnp.bfloat16)
```

```python
import functools
import math

import jax
import jax.numpy as jnp
from jax import lax
import numpy as np
from jax.experimental import pallas as pl
from jax.experimental.pallas import tpu as pltpu
from jax.sharding import PartitionSpec as P

BLOCK = 128
EXPERTS = 32
TOP = 2
CAP = 2
EXP_GROUP = 8


HIGHEST = lax.Precision.HIGHEST
RESIDUAL_SCALE = math.sqrt(2.0)
NORM_EPS = 1e-05
GROUP_EPS = 1e-06
ROPE_BASE = 10000.0


def entering(array, axis, join, neutral, backward):
    count = lax.axis_size(axis)
    place = lax.axis_index(axis)
    ahead = count - 1 - place if backward else place
    gathered = jax.tree.map(
        lambda a, kind: lax.all_gather(a.astype(kind), axis),
        array,
        jax.tree.map(lambda a: jnp.bfloat16 if a.dtype == jnp.float32 else a.dtype, array),
    )
    state = jax.tree.map(lambda a, e: jnp.zeros_like(a) + jnp.asarray(e, a.dtype), array, neutral)

    def one(hop, state):
        source = count - 1 - hop if backward else hop
        return join(
            state,
            jax.tree.map(
                lambda a, own: lax.dynamic_index_in_dim(a, source, 0, False).astype(own.dtype),
                gathered,
                array,
            ),
        )

    return lax.fori_loop(0, ahead, one, state)


def rotate(vectors, token_positions):
    half_width = vectors.shape[-1] // 2
    frequencies = ROPE_BASE ** (-jnp.arange(half_width, dtype=jnp.float32) / half_width)
    angles = token_positions.astype(jnp.float32)[:, None] * frequencies[None, :]
    cosine = jnp.cos(angles)[:, None, :]
    sine_part = jnp.sin(angles)[:, None, :]
    first_half = vectors[..., :half_width].astype(jnp.float32)
    second = vectors[..., half_width:].astype(jnp.float32)
    return jnp.concatenate(
        [first_half * cosine - second * sine_part, first_half * sine_part + second * cosine],
        axis=-1,
    )


def prepare(query_w, key_w, value_w, number_of_heads, token_positions):
    length = query_w.shape[0]
    queries_f = rotate(query_w.reshape(length, number_of_heads, -1), token_positions)
    key_dim = queries_f.shape[-1]
    queries = queries_f.astype(jnp.bfloat16)
    keys_rot = (
        rotate(key_w.reshape(length, number_of_heads, -1), token_positions)
        * (1.0 / math.sqrt(key_dim))
    ).astype(jnp.bfloat16)
    values = value_w.reshape(length, number_of_heads, -1)
    return (queries, keys_rot, values)


def sweep_blocks(queries, keys_rot, values, log_decay, strict, state_init, span_size):
    length, number_of_heads, key_dim = queries.shape
    value_dim = values.shape[-1]
    block_count = length // span_size

    def split_blocks(array):
        return array.reshape(block_count, span_size, number_of_heads, array.shape[-1])

    decay_blocks = log_decay.reshape(number_of_heads, block_count, span_size).transpose(1, 0, 2)
    position_index = jnp.arange(span_size)
    if strict:
        allowed = position_index[:, None] > position_index[None, :]
    else:
        allowed = position_index[:, None] >= position_index[None, :]

    def advance(state_now, inputs):
        query_blk, key_blk, value_blk, decay_blk = inputs
        cumulative = jnp.cumsum(decay_blk, axis=1)
        log_gap = cumulative[:, :, None] - cumulative[:, None, :]
        weights = jnp.where(allowed[None], jnp.exp(jnp.where(allowed[None], log_gap, 0.0)), 0.0)
        scores = (
            jnp.einsum("ihd,jhd->hij", query_blk, key_blk, preferred_element_type=jnp.float32)
            * weights
        )
        weighted = scores.astype(jnp.bfloat16)
        inner_part = jnp.einsum(
            "hij,jhv->ihv", weighted, value_blk, preferred_element_type=jnp.float32
        )
        carried = (
            jnp.einsum("ihd,hdv->ihv", query_blk.astype(jnp.float32), state_now, precision=HIGHEST)
            * jnp.exp(cumulative).T[:, :, None]
        )
        key_scaled = (
            key_blk.astype(jnp.float32) * jnp.exp(cumulative[:, -1:] - cumulative).T[:, :, None]
        )
        state_next = state_now * jnp.exp(cumulative[:, -1])[:, None, None] + jnp.einsum(
            "jhd,jhv->hdv", key_scaled, value_blk.astype(jnp.float32), precision=HIGHEST
        )
        return (state_next, inner_part + carried)

    final_state, outputs = lax.scan(
        advance,
        state_init,
        (split_blocks(queries), split_blocks(keys_rot), split_blocks(values), decay_blocks),
    )
    return (outputs.reshape(length, number_of_heads, value_dim), final_state)


def summary(keys_rot, values, log_decay):
    cumulative = jnp.cumsum(log_decay, axis=1)
    key_scaled = (
        keys_rot.astype(jnp.float32) * jnp.exp(cumulative[:, -1:] - cumulative).T[:, :, None]
    )
    return (
        jnp.exp(cumulative[:, -1]),
        jnp.einsum("lhd,lhv->hdv", key_scaled, values.astype(jnp.float32), precision=HIGHEST),
    )


def chain_states(earlier, later):
    decay_a0, state_a0, decay_b0, state_b0 = earlier
    decay_a1, state_a1, decay_b1, state_b1 = later
    return (
        decay_a0 * decay_a1,
        state_a0 * decay_a1[:, None, None] + state_a1,
        decay_b0 * decay_b1,
        state_b0 * decay_b1[:, None, None] + state_b1,
    )


def neutral(parts):
    return (
        jnp.ones_like(parts[0]),
        jnp.zeros_like(parts[1]),
        jnp.ones_like(parts[2]),
        jnp.zeros_like(parts[3]),
    )


def carry_states(forward_parts, backward_parts):
    into_forward = entering(forward_parts, "sp", chain_states, neutral(forward_parts), False)
    into_backward = entering(backward_parts, "sp", chain_states, neutral(backward_parts), True)
    return (into_forward, into_backward)


def finish(forward, backward_flipped):
    total_sum = forward + backward_flipped[::-1]
    normed = total_sum * lax.rsqrt(
        jnp.mean(total_sum * total_sum, axis=-1, keepdims=True) + GROUP_EPS
    )
    return normed.reshape(total_sum.shape[0], -1).astype(jnp.bfloat16)


def layer_norm(stream, gain):
    center = stream - jnp.mean(stream, axis=-1, keepdims=True)
    spread = jnp.mean(center * center, axis=-1, keepdims=True)
    return center * lax.rsqrt(spread + NORM_EPS) * gain


def slot_table(expert_ids):
    onehot = (expert_ids[..., None] == jnp.arange(EXPERTS, dtype=jnp.int32)).astype(jnp.int32)
    earlier = jnp.cumsum(onehot, axis=-2) - onehot
    rank_order = jnp.sum(earlier * onehot, axis=-1)
    kept_mask = rank_order < CAP
    slot_index = expert_ids * CAP + jnp.minimum(rank_order, CAP - 1)
    return (slot_index, kept_mask)


def gate_up(rows, gate_w, up_w):
    gate_part = jnp.einsum("xecd,edf->xecf", rows, gate_w, preferred_element_type=jnp.float32)
    up_part = jnp.einsum("xecd,edf->xecf", rows, up_w, preferred_element_type=jnp.float32)
    return (jax.nn.silu(gate_part) * up_part).astype(jnp.bfloat16)


def shards(
    query_a,
    key_a,
    value_a,
    decay_a,
    query_b,
    key_b,
    value_b,
    decay_b,
    out_weight_a,
    out_weight_b,
    residual,
    norm_gain,
    route_group,
    route_expert,
    route_weight,
    expert_gate,
    expert_up,
    expert_down,
):
    length = query_a.shape[0]
    token_positions = lax.axis_index("sp") * length + jnp.arange(length, dtype=jnp.int32)
    heads_a = decay_a.shape[1]
    heads_b = decay_b.shape[1]
    qa_rot, ka_rot, va_all = prepare(query_a, key_a, value_a, heads_a, token_positions)
    qb_rot, kb_rot, vb_all = prepare(query_b, key_b, value_b, heads_b, token_positions)
    flip_a = (qa_rot[::-1], ka_rot[::-1], va_all[::-1], decay_a[1][:, ::-1])
    flip_b = (qb_rot[::-1], kb_rot[::-1], vb_all[::-1], decay_b[1][:, ::-1])
    forward_parts = summary(ka_rot, va_all, decay_a[0]) + summary(kb_rot, vb_all, decay_b[0])
    backward_parts = summary(flip_a[1], flip_a[2], flip_a[3]) + summary(
        flip_b[1], flip_b[2], flip_b[3]
    )
    into_forward, into_backward = carry_states(forward_parts, backward_parts)
    forward_a = sweep_blocks(qa_rot, ka_rot, va_all, decay_a[0], False, into_forward[1], BLOCK)[0]
    forward_b = sweep_blocks(qb_rot, kb_rot, vb_all, decay_b[0], False, into_forward[3], BLOCK)[0]
    backward_a = sweep_blocks(
        flip_a[0], flip_a[1], flip_a[2], flip_a[3], True, into_backward[1], BLOCK
    )[0]
    backward_b = sweep_blocks(
        flip_b[0], flip_b[1], flip_b[2], flip_b[3], True, into_backward[3], BLOCK
    )[0]
    mixed_a = finish(forward_a, backward_a)
    mixed_b = finish(forward_b, backward_b)
    rows_dev = length // lax.axis_size("tp")
    mix = lax.psum_scatter(
        (
            jnp.dot(mixed_a, out_weight_a, preferred_element_type=jnp.float32)
            + jnp.dot(mixed_b, out_weight_b, preferred_element_type=jnp.float32)
        ).astype(jnp.bfloat16),
        "tp",
        scatter_dimension=0,
        tiled=True,
    ).astype(jnp.float32)
    hidden_in = layer_norm(
        RESIDUAL_SCALE * residual.astype(jnp.float32) + mix, norm_gain[0]
    ).astype(jnp.bfloat16)
    width = hidden_in.shape[1]
    ffn_width = expert_gate.shape[2]
    sp_count = lax.axis_size("sp")
    per_device = EXPERTS // sp_count
    slots = EXPERTS * CAP
    global_ids = (route_group[:, None] * EXP_GROUP + route_expert).reshape(-1)
    slot_index, kept_mask = slot_table(global_ids)
    hits = (slot_index[:, None] == jnp.arange(slots, dtype=jnp.int32)[None, :]) & kept_mask[:, None]
    choose = jnp.sum(hits.reshape(rows_dev, TOP, slots).astype(jnp.int32), axis=1).astype(
        jnp.bfloat16
    )
    outgoing = jnp.einsum(
        "rs,rd->sd", choose, hidden_in, preferred_element_type=jnp.float32
    ).astype(jnp.bfloat16)
    outgoing = outgoing.reshape(sp_count, per_device * CAP, width)
    received = lax.all_to_all(outgoing, "sp", split_axis=0, concat_axis=0, tiled=True)
    piece_rows = lax.all_gather(received, "tp", axis=0, tiled=True)
    piece_count = piece_rows.shape[0]
    shaped = piece_rows.reshape(-1, per_device, CAP, width)
    hidden = gate_up(shaped, expert_gate, expert_up).reshape(
        piece_count, per_device * CAP, ffn_width
    )
    flat_hidden = hidden.reshape(-1, ffn_width)
    piece_rows = flat_hidden.reshape(-1, per_device, CAP, ffn_width)
    summed = lax.psum_scatter(
        jnp.einsum("xecf,efd->xecd", piece_rows, expert_down, preferred_element_type=jnp.float32)
        .reshape(lax.axis_size("tp") * (sp_count * per_device * CAP), width)
        .astype(jnp.bfloat16),
        "tp",
        scatter_dimension=0,
        tiled=True,
    )
    back_rows = summed.reshape(sp_count, per_device * CAP, width)
    returned = lax.all_to_all(back_rows, "sp", split_axis=0, concat_axis=0, tiled=True).reshape(
        slots, width
    )
    picked = (
        jnp.take(returned, slot_index, axis=0).astype(jnp.float32).reshape(rows_dev, TOP, width)
    )
    factor = jnp.where(kept_mask.reshape(rows_dev, TOP), route_weight, 0.0)
    ffn = jnp.sum(picked * factor[..., None], axis=1)
    return layer_norm(RESIDUAL_SCALE * hidden_in.astype(jnp.float32) + ffn, norm_gain[1]).astype(
        jnp.bfloat16
    )


MESH = pl.DeviceIdType.MESH
F32 = jnp.float32
BF16 = jnp.bfloat16
NT = (((1,), (1,)), ((), ()))
TN = (((0,), (0,)), ((), ()))
LANES = 128


def dot(a, b, dims=None, precision=None):
    dims = dims or (((1,), (0,)), ((), ()))
    return lax.dot_general(a, b, dims, precision=precision, preferred_element_type=F32)


def layer_kernel(
    cfg,
    qa,
    ka,
    va,
    qb,
    kb,
    vb,
    dec,
    cos_a,
    sin_a,
    cos_b,
    sin_b,
    head_mask,
    block_mask,
    rope_perm,
    sort_rows,
    unsort_rows,
    woa,
    wob,
    res,
    gain,
    rg,
    re,
    rw,
    eg,
    eu,
    ed,
    out,
    wo_v,
    eg_v,
    eu_v,
    ed_v,
    qa_s,
    ka_s,
    qb_s,
    kb_s,
    acc_a,
    acc_b,
    mixed,
    loc,
    loc_b,
    dfs,
    dfs_b,
    cin,
    cin_b,
    cout,
    cout_b,
    p_out,
    p_in,
    x_out,
    x_in,
    own,
    gbuf,
    obuf,
    xs,
    ys,
    ep_out,
    ep_in,
    ex_out,
    ex_in,
    ret,
    fin,
    w_sem,
    wo_sem,
    c_send,
    c_recv,
    cb_send,
    cb_recv,
    p_send,
    p_recv,
    x_send,
    x_recv,
    d_send,
    g_send,
    g_recv,
    ep_send,
    ep_recv,
    ex_send,
    ex_recv,
    r_send,
    r_recv,
):
    nsp, ntp, ha, hb = cfg["nsp"], cfg["ntp"], cfg["ha"], cfg["hb"]
    half = ntp // 2
    length, width = qa.shape[0], res.shape[1]
    dka, dva = qa.shape[1] // ha, va.shape[1] // ha
    dkb = qb.shape[1] // hb
    rows = length // ntp
    cph = dva // LANES
    chunks = ha * cph
    sp, tp = lax.axis_index("sp"), lax.axis_index("tp")
    pair = tp // 2
    core = tp % 2
    mate = 2 * pair + 1 - core
    per_dev = eg.shape[0]
    tiles = p_out.shape[0]
    tile = width // tiles

    wo_copies = [
        pltpu.make_async_copy(woa, wo_v.at[pl.ds(0, ha * dva)], wo_sem.at[0]),
        pltpu.make_async_copy(wob, wo_v.at[pl.ds(ha * dva, wob.shape[0])], wo_sem.at[1]),
    ]
    for c in wo_copies:
        c.start()

    def weight_copies(e):
        return [
            pltpu.make_async_copy(a.at[e], b.at[e], w_sem.at[i, e])
            for i, (a, b) in enumerate(((eg, eg_v), (eu, eu_v), (ed, ed_v)))
        ]

    @pl.loop(0, per_dev)
    def _(e):
        for c in weight_copies(e):
            c.start()

    barrier = pltpu.get_barrier_semaphore()
    for d in range(1, nsp):
        pl.semaphore_signal(
            barrier, inc=1, device_id={"sp": (sp + d) % nsp}, device_id_type=MESH
        )
    for d in range(1, ntp):
        pl.semaphore_signal(
            barrier, inc=1, device_id={"tp": (tp + d) % ntp}, device_id_type=MESH
        )

    def remote(src, dst, ssem, rsem, axis, where):
        return pltpu.make_async_remote_copy(
            src_ref=src,
            dst_ref=dst,
            send_sem=ssem,
            recv_sem=rsem,
            device_id={axis: where},
            device_id_type=MESH,
        )

    r_i = lax.broadcasted_iota(jnp.int32, (length, length), 0)
    c_i = lax.broadcasted_iota(jnp.int32, (length, length), 1)
    lower = r_i >= c_i
    tri = jnp.where(lower, 1.0, 0.0).astype(F32)
    tri_s = jnp.where(r_i > c_i, 1.0, 0.0).astype(F32)
    d = dec[...]
    inc_col = dot(tri, d, NT, HIGHEST)
    inc_row = dot(d, tri, NT, HIGHEST)
    exc_col = dot(tri_s, d, NT, HIGHEST)
    exc_row = dot(d, tri_s, NT, HIGHEST)
    total = inc_row[:, length - 1 : length]

    def index(kind, back, h):
        return (0 if kind == "a" else 2 * ha) + (hb if kind == "b" else ha) * back + h

    def tot(kind, back, h):
        i = index(kind, back, h)
        return total[i : i + 1, :]

    def col(arr, kind, back, h):
        i = index(kind, back, h)
        return arr[:, i : i + 1]

    def row(arr, kind, back, h):
        i = index(kind, back, h)
        return arr[i : i + 1, :]

    hw = dka // 2
    ca, sa = cos_a[...], sin_a[...]

    def rot_a(x, scale):
        x1, x2 = x[:, :hw].astype(F32), x[:, hw:].astype(F32)
        y = jnp.concatenate([x1 * ca - x2 * sa, x1 * sa + x2 * ca], axis=1)
        return (y * scale).astype(BF16)

    masks = [head_mask[j : j + 1, :] for j in range(hb)]
    bm = block_mask[...]
    vbv = vb[...]

    def rot_b(x, scale):
        y = x.astype(F32) * cos_b[...] + dot(x, rope_perm[...]) * sin_b[...]
        return (y * scale).astype(BF16)

    def spread(cols):
        return functools.reduce(lambda x, y: x + y, [c * m for c, m in zip(cols, masks)])

    kbr = rot_b(kb[...], 1.0 / math.sqrt(dkb))
    kb_s[...] = kbr
    for back in (0, 1):
        if back:
            scale = spread([jnp.exp(col(exc_col, "b", 1, j)) for j in range(hb)])
        else:
            scale = spread(
                [jnp.exp(tot("b", 0, j) - col(inc_col, "b", 0, j)) for j in range(hb)]
            )
        full = dot((kbr.astype(F32) * scale).astype(BF16), vbv, TN) * bm
        loc_b[back] = functools.reduce(
            lambda x, y: x + y, [full[j * dkb : (j + 1) * dkb] for j in range(hb)]
        )
        dfs_b[back] = jnp.broadcast_to(
            spread([jnp.exp(tot("b", back, j)) for j in range(hb)]), dfs_b.shape[1:]
        )
    for h in range(ha):
        k = rot_a(ka[:, h * dka : (h + 1) * dka], 1.0 / math.sqrt(dka))
        ka_s[:, h * dka : (h + 1) * dka] = k
        kf = k.astype(F32)
        for back in (0, 1):
            if back:
                scale = jnp.exp(col(exc_col, "a", 1, h))
            else:
                scale = jnp.exp(tot("a", 0, h) - col(inc_col, "a", 0, h))
            state = dot((kf * scale).astype(BF16), va[:, h * dva : (h + 1) * dva], TN)
            for c in range(cph):
                loc[back, h * cph + c] = state[:, c * LANES : (c + 1) * LANES]
                dfs[back, h * cph + c] = jnp.broadcast_to(
                    jnp.exp(tot("a", back, h)), dfs.shape[2:]
                )

    pl.semaphore_wait(barrier, nsp - 1 + ntp - 1)

    @pl.when(sp == 0)
    def _():
        cin[0] = jnp.zeros(cin.shape[1:], BF16)
        cin_b[0] = jnp.zeros(cin_b.shape[1:], BF16)

    @pl.when(sp == nsp - 1)
    def _():
        cin[1] = jnp.zeros(cin.shape[1:], BF16)
        cin_b[1] = jnp.zeros(cin_b.shape[1:], BF16)

    def chain_copy(back, c):
        to = (sp + nsp - 1) % nsp if back else (sp + 1) % nsp
        return remote(
            cout.at[back, c], cin.at[back, c], c_send.at[back, c], c_recv.at[back, c], "sp", to
        )

    def chain_copy_b(back):
        to = (sp + nsp - 1) % nsp if back else (sp + 1) % nsp
        return remote(
            cout_b.at[back], cin_b.at[back], cb_send.at[back], cb_recv.at[back], "sp", to
        )

    def chain(back, t):
        place = nsp - 1 - sp if back else sp
        c = t - place

        @pl.when((c >= 0) & (c < chunks))
        def _():
            @pl.when(place > 0)
            def _():
                chain_copy(back, c).wait_recv()

            @pl.when(place < nsp - 1)
            def _():
                cout[back, c] = (
                    cin[back, c].astype(F32) * dfs[back, c][:1] + loc[back, c]
                ).astype(BF16)
                chain_copy(back, c).start()

        @pl.when(c == 0)
        def _():
            @pl.when(place > 0)
            def _():
                chain_copy_b(back).wait_recv()

            @pl.when(place < nsp - 1)
            def _():
                cout_b[back] = (
                    cin_b[back].astype(F32) * dfs_b[back][:1] + loc_b[back]
                ).astype(BF16)
                chain_copy_b(back).start()

    def weights(kind, h):
        ahead = col(inc_col, kind, 0, h) - row(inc_row, kind, 0, h)
        behind = row(exc_row, kind, 1, h) - col(exc_col, kind, 1, h)
        return jnp.exp(jnp.minimum(jnp.where(lower, ahead, behind), 0.0))

    def local_a(h):
        q = rot_a(qa[:, h * dka : (h + 1) * dka], 1.0)
        qa_s[:, h * dka : (h + 1) * dka] = q
        s = dot(q, ka_s[:, h * dka : (h + 1) * dka], NT) * weights("a", h)
        acc_a[:, h * dva : (h + 1) * dva] = dot(
            s.astype(BF16), va[:, h * dva : (h + 1) * dva]
        )

    def local_b(j):
        if j == 0:
            qb_s[...] = rot_b(qb[...], 1.0)
        q = (qb_s[...].astype(F32) * masks[j]).astype(BF16)
        s = dot(q, kb_s[...], NT) * weights("b", j)
        part = dot(s.astype(BF16), vb[...]) * masks[j]
        if j:
            acc_b[...] += part
        else:
            acc_b[...] = part

    work = [functools.partial(local_a, h) for h in range(ha)]
    work += [functools.partial(local_b, j) for j in range(hb)]
    steps = chunks + nsp - 1
    for t in range(steps):
        chain(0, t)
        chain(1, t)
        if t < len(work):
            work[t]()
    for piece in work[steps:]:
        piece()

    for h in range(ha):
        q = qa_s[:, h * dka : (h + 1) * dka]
        parts = []
        for back in (0, 1):
            state = jnp.concatenate([cin[back, h * cph + c] for c in range(cph)], axis=1)
            if back:
                scale = jnp.exp(tot("a", 1, h) - col(exc_col, "a", 1, h))
            else:
                scale = jnp.exp(col(inc_col, "a", 0, h))
            parts.append(dot(q, state) * scale)
        y = acc_a[:, h * dva : (h + 1) * dva] + parts[0] + parts[1]
        y = y * lax.rsqrt(jnp.mean(y * y, axis=-1, keepdims=True) + GROUP_EPS)
        mixed[:, h * dva : (h + 1) * dva] = y.astype(BF16)
    y = acc_b[...]
    for back in (0, 1):
        state = jnp.concatenate([cin_b[back].astype(F32)] * hb, axis=0) * bm
        if back:
            scale = spread([jnp.exp(tot("b", 1, j) - col(exc_col, "b", 1, j)) for j in range(hb)])
        else:
            scale = spread([jnp.exp(col(inc_col, "b", 0, j)) for j in range(hb)])
        y = y + dot(qb_s[...], state.astype(BF16)) * scale
    square = dot(y * y, bm, None, HIGHEST) * (1.0 / dkb)
    mixed[:, ha * dva :] = (y * lax.rsqrt(square + GROUP_EPS)).astype(BF16)

    for c in wo_copies:
        c.wait()

    def block(i):
        return mixed[pl.ds(pl.multiple_of(i * rows, rows), rows), :]

    theirs = jnp.concatenate([block(2 * i + 1 - core) for i in range(half)], axis=0)
    mine = jnp.concatenate([block(2 * i + core) for i in range(half)], axis=0)

    def p_copy(n):
        return remote(p_out.at[n], p_in.at[n], p_send.at[n], p_recv.at[n], "tp", mate)

    def x_copy(n, k):
        i = (pair + k) % half
        return remote(
            x_out.at[k - 1, n],
            x_in.at[k - 1, n],
            x_send.at[k - 1, n],
            x_recv.at[k - 1, n],
            "tp",
            2 * i + core,
        )

    for n in range(tiles):
        p_out[n] = dot(theirs, wo_v[:, n * tile : (n + 1) * tile]).astype(BF16)
        p_copy(n).start()
    for n in range(tiles):
        own[n] = dot(mine, wo_v[:, n * tile : (n + 1) * tile])
        p_copy(n).wait_recv()
        own[n] += p_in[n].astype(F32)
        for k in range(1, half):
            i = (pair + k) % half
            x_out[k - 1, n] = own[n, pl.ds(pl.multiple_of(i * rows, rows), rows), :].astype(BF16)
            x_copy(n, k).start()
    mix = []
    for n in range(tiles):
        m = own[n, pl.ds(pl.multiple_of(pair * rows, rows), rows), :]
        for k in range(1, half):
            x_copy(n, k).wait_recv()
            m = m + x_in[k - 1, n].astype(F32)
        mix.append(m)
    mix = jnp.concatenate(mix, axis=1)

    def norm(x, g):
        x = x - jnp.mean(x, axis=-1, keepdims=True)
        return x * lax.rsqrt(jnp.mean(x * x, axis=-1, keepdims=True) + NORM_EPS) * g

    hidden = norm(RESIDUAL_SCALE * res[...].astype(F32) + mix, gain[0:1, :]).astype(BF16)

    slots = EXPERTS * CAP
    lane_e = lax.broadcasted_iota(jnp.int32, (rows, EXPERTS), 1)
    lane_s = lax.broadcasted_iota(jnp.int32, (rows, slots), 1)
    ids = [rg[...] * EXP_GROUP + re[:, k : k + 1] for k in range(TOP)]
    hot = [jnp.where(i == lane_e, 1.0, 0.0) for i in ids]
    before = jnp.where(
        lax.broadcasted_iota(jnp.int32, (rows, rows), 0)
        > lax.broadcasted_iota(jnp.int32, (rows, rows), 1),
        1.0,
        0.0,
    )
    earlier = dot(before.astype(BF16), functools.reduce(jnp.add, hot).astype(BF16))
    choose = []
    for i, o in zip(ids, hot):
        rank = jnp.sum(earlier * o, axis=1, keepdims=True)
        hit = jnp.zeros((rows, slots), F32)
        for c in range(CAP):
            hit = hit + jnp.where((lane_s == i * CAP + c) & (rank == float(c)), 1.0, 0.0)
        choose.append(hit)
    outgoing = dot(functools.reduce(jnp.add, choose).astype(BF16), hidden, TN).astype(BF16)
    piece = per_dev * CAP
    for s in range(nsp):
        obuf[s] = outgoing[s * piece : (s + 1) * piece]

    def d_copy(k):
        to = (sp + k) % nsp
        return remote(
            obuf.at[to], gbuf.at[tp, sp], d_send.at[k - 1], g_recv.at[tp, sp], "sp", to
        )

    def g_copy(t, s, to, which, k):
        return remote(
            gbuf.at[t, s], gbuf.at[t, s], g_send.at[which, k], g_recv.at[t, s], "tp", to
        )

    def relay(s, k):
        for j in range(1, half):
            g_copy(tp, s, 2 * ((pair + j) % half) + core, j, k).start()
        g_copy(tp, s, mate, 0, k).start()

    order = sorted(range(1, nsp), key=lambda k: -min(k, nsp - k))
    for k in order:
        d_copy(k).start()
    gbuf[tp, sp] = obuf[sp]
    relay(sp, 0)
    for k in range(1, nsp):
        s = (sp + k) % nsp
        g_copy(tp, s, mate, 0, k).wait_recv()
        relay(s, k)
    for k in range(nsp):
        s = (sp + k) % nsp
        for j in range(1, half):
            t = 2 * ((pair + j) % half) + core
            g_copy(t, s, mate, 0, k).wait_recv()
            g_copy(t, s, mate, half + j - 1, k).start()
    for i in range(half):
        for k in range(nsp):
            g_copy(2 * i + 1 - core, (sp + k) % nsp, mate, 0, k).wait_recv()

    count = ntp * nsp * piece
    stack = count // per_dev
    xs[...] = dot(sort_rows[...], gbuf[...].reshape(count, width)).astype(BF16)

    @pl.loop(0, per_dev)
    def _(e):
        for c in weight_copies(e):
            c.wait()
        at = pl.ds(pl.multiple_of(e * stack, stack), stack)
        x = xs[at, :]
        g = dot(x, eg_v[e])
        u = dot(x, eu_v[e])
        h = (g / (1.0 + jnp.exp(-g)) * u).astype(BF16)
        ys[at, :] = dot(h, ed_v[e]).astype(BF16)

    def ep_copy(k):
        return remote(ep_out.at[k], ep_in.at[k], ep_send.at[k], ep_recv.at[k], "tp", mate)

    def ex_copy(k):
        to = 2 * ((pair + k) % half) + core
        return remote(
            ex_out.at[k - 1], ex_in.at[k - 1], ex_send.at[k - 1], ex_recv.at[k - 1], "tp", to
        )

    turn = list(range(1, half)) + [0]
    for k in turn:
        i = (pair + k) % half
        ep_out[k] = dot(unsort_rows[2 * i + 1 - core], ys[...]).astype(BF16)
        ep_copy(k).start()
    for k in turn:
        i = (pair + k) % half
        z = dot(unsort_rows[2 * i + core], ys[...])
        ep_copy(k).wait_recv()
        z = z + ep_in[k].astype(F32)
        if k:
            ex_out[k - 1] = z.astype(BF16)
            ex_copy(k).start()
    for k in range(1, half):
        ex_copy(k).wait_recv()
        z = z + ex_in[k - 1].astype(F32)
    z = z.astype(BF16)
    for s in range(nsp):
        fin[s] = z[s * piece : (s + 1) * piece]

    def r_copy(k):
        to = (sp + k) % nsp
        return remote(fin.at[to], ret.at[sp], r_send.at[k - 1], r_recv.at[sp], "sp", to)

    def r_arrival(k):
        s = (sp + k) % nsp
        return remote(fin.at[s], ret.at[s], r_send.at[k - 1], r_recv.at[s], "sp", s)

    for k in order:
        r_copy(k).start()
    ret[sp] = fin[sp]
    factor = jnp.zeros((rows, slots), F32)
    for k in range(TOP):
        factor = factor + choose[k] * rw[:, k : k + 1]
    high = factor.astype(BF16)
    low = (factor - high.astype(F32)).astype(BF16)
    for k in range(1, nsp):
        r_arrival(k).wait_recv()
    back_rows = ret[...].reshape(slots, width)
    ffn = dot(high, back_rows) + dot(low, back_rows)
    out[...] = norm(RESIDUAL_SCALE * hidden.astype(F32) + ffn, gain[1:2, :]).astype(BF16)

    for back in (0, 1):
        place = nsp - 1 - sp if back else sp

        @pl.when(place < nsp - 1)
        def _():
            chain_copy_b(back).wait_send()
            for c in range(chunks):
                chain_copy(back, c).wait_send()

    for n in range(tiles):
        p_copy(n).wait_send()
        for k in range(1, half):
            x_copy(n, k).wait_send()
    for k in range(1, nsp):
        d_copy(k).wait_send()
        r_copy(k).wait_send()
    for k in range(nsp):
        for which in range(2 * half - 1):
            g_copy(tp, sp, mate, which, k).wait_send()
    for k in range(half):
        ep_copy(k).wait_send()
    for k in range(1, half):
        ex_copy(k).wait_send()


def fits(mesh_sizes, heads_b, width_b, experts_here, rows):
    nsp, ntp = mesh_sizes
    aligned = (experts_here * CAP) % 16 == 0 and rows % 16 == 0 and heads_b * 64 % 128 == 0
    return ntp % 2 == 0 and ntp >= 4 and nsp >= 2 and aligned


def fused(
    query_a,
    key_a,
    value_a,
    decay_a,
    query_b,
    key_b,
    value_b,
    decay_b,
    out_weight_a,
    out_weight_b,
    residual,
    norm_gain,
    route_group,
    route_expert,
    route_weight,
    expert_gate,
    expert_up,
    expert_down,
):
    nsp, ntp = lax.axis_size("sp"), lax.axis_size("tp")
    length = query_a.shape[0]
    rows, width = residual.shape
    ha, hb = decay_a.shape[1], decay_b.shape[1]
    dka, dva = query_a.shape[1] // ha, value_a.shape[1] // ha
    dkb, wb = query_b.shape[1] // hb, query_b.shape[1]
    per_dev, _, ff = expert_gate.shape
    piece = per_dev * CAP
    half = ntp // 2
    chunks = ha * dva // LANES
    heads = 2 * (ha + hb)
    dec = jnp.concatenate([decay_a.reshape(2 * ha, length), decay_b.reshape(2 * hb, length)])
    positions = (lax.axis_index("sp") * length + jnp.arange(length, dtype=jnp.int32)).astype(F32)

    def angles(hw):
        freq = ROPE_BASE ** (-jnp.arange(hw, dtype=F32) / hw)
        return positions[:, None] * freq[None, :]

    ang_a = angles(dka // 2)
    ang_b = angles(dkb // 2)
    cos_b, sin_b = jnp.cos(ang_b), jnp.sin(ang_b)
    cos_b = jnp.tile(cos_b, (1, 2 * hb))
    sin_b = jnp.tile(sin_b, (1, 2 * hb))
    lane = np.arange(wb)
    head_mask = (lane[None, :] // dkb == np.arange(hb)[:, None]).astype(np.float32)
    block_mask = (lane[None, :] // dkb == lane[:, None] // dkb).astype(np.float32)
    first = lane % dkb < dkb // 2
    perm = np.zeros((wb, wb), np.float32)
    perm[np.where(first, lane + dkb // 2, lane - dkb // 2), lane] = np.where(first, -1.0, 1.0)
    count = ntp * nsp * piece
    o = np.arange(count)
    stack = count // per_dev
    source = (o % stack) // CAP * piece + o // stack * CAP + o % CAP
    sort_rows = np.zeros((count, count), np.float32)
    sort_rows[o, source] = 1.0
    unsort_rows = sort_rows.T.reshape(ntp, nsp * piece, count)
    tiles = 4 if width % 512 == 0 else 1
    tile = width // tiles
    vmem = pl.BlockSpec(memory_space=pltpu.VMEM)
    hbm = pl.BlockSpec(memory_space=pl.ANY)
    dma = pltpu.SemaphoreType.DMA
    V = pltpu.VMEM
    return pl.pallas_call(
        functools.partial(layer_kernel, {"nsp": nsp, "ntp": ntp, "ha": ha, "hb": hb}),
        out_shape=jax.ShapeDtypeStruct((rows, width), BF16),
        in_specs=[vmem] * 16 + [hbm] * 2 + [vmem] * 5 + [hbm] * 3,
        out_specs=vmem,
        scratch_shapes=[
            V((out_weight_a.shape[0] + out_weight_b.shape[0], width), BF16),
            V(expert_gate.shape, BF16),
            V(expert_up.shape, BF16),
            V(expert_down.shape, BF16),
            V((length, ha * dka), BF16),
            V((length, ha * dka), BF16),
            V((length, wb), BF16),
            V((length, wb), BF16),
            V((length, ha * dva), F32),
            V((length, wb), F32),
            V((length, ha * dva + wb), BF16),
            V((2, chunks, dka, LANES), F32),
            V((2, dkb, wb), F32),
            V((2, chunks, 8, LANES), F32),
            V((2, 8, wb), F32),
            V((2, chunks, dka, LANES), BF16),
            V((2, dkb, wb), BF16),
            V((2, chunks, dka, LANES), BF16),
            V((2, dkb, wb), BF16),
            V((tiles, half * rows, tile), BF16),
            V((tiles, half * rows, tile), BF16),
            V((half - 1, tiles, rows, tile), BF16),
            V((half - 1, tiles, rows, tile), BF16),
            V((tiles, half * rows, tile), F32),
            V((ntp, nsp, piece, width), BF16),
            V((nsp, piece, width), BF16),
            V((count, width), BF16),
            V((count, width), BF16),
            V((half, nsp * piece, width), BF16),
            V((half, nsp * piece, width), BF16),
            V((half - 1, nsp * piece, width), BF16),
            V((half - 1, nsp * piece, width), BF16),
            V((nsp, piece, width), BF16),
            V((nsp, piece, width), BF16),
            dma((3, per_dev)),
            dma((2,)),
            dma((2, chunks)),
            dma((2, chunks)),
            dma((2,)),
            dma((2,)),
            dma((tiles,)),
            dma((tiles,)),
            dma((half - 1, tiles)),
            dma((half - 1, tiles)),
            dma((nsp - 1,)),
            dma((2 * half - 1, nsp)),
            dma((ntp, nsp)),
            dma((half,)),
            dma((half,)),
            dma((half - 1,)),
            dma((half - 1,)),
            dma((nsp - 1,)),
            dma((nsp,)),
        ],
        compiler_params=pltpu.CompilerParams(
            collective_id=0, has_side_effects=True, vmem_limit_bytes=60 * 1024 * 1024
        ),
    )(
        query_a,
        key_a,
        value_a,
        query_b,
        key_b,
        value_b,
        dec,
        jnp.cos(ang_a),
        jnp.sin(ang_a),
        cos_b,
        sin_b,
        jnp.asarray(head_mask),
        jnp.asarray(block_mask),
        jnp.asarray(perm, BF16),
        jnp.asarray(sort_rows, BF16),
        jnp.asarray(unsort_rows, BF16),
        out_weight_a,
        out_weight_b,
        residual,
        norm_gain,
        route_group[:, None],
        route_expert,
        route_weight,
        expert_gate,
        expert_up,
        expert_down,
    )


def layer(*args):
    sizes = (lax.axis_size("sp"), lax.axis_size("tp"))
    heads_b, experts_here, rows = args[7].shape[1], args[15].shape[0], args[10].shape[0]
    if fits(sizes, heads_b, args[4].shape[1], experts_here, rows):
        return fused(*args)
    return shards(*args)


def solution(mesh):
    return jax.shard_map(
        layer,
        mesh=mesh,
        in_specs=(
            P(("grp", "sp"), "tp"),
            P(("grp", "sp"), "tp"),
            P(("grp", "sp"), "tp"),
            P(None, "tp", ("grp", "sp")),
            P(("grp", "sp"), "tp"),
            P(("grp", "sp"), "tp"),
            P(("grp", "sp"), "tp"),
            P(None, "tp", ("grp", "sp")),
            P("tp", None),
            P("tp", None),
            P(("grp", "sp", "tp"), None),
            P(),
            P(("grp", "sp", "tp")),
            P(("grp", "sp", "tp"), None),
            P(("grp", "sp", "tp"), None),
            P("sp", None, "tp"),
            P("sp", None, "tp"),
            P("sp", "tp", None),
        ),
        out_specs=P(("grp", "sp", "tp"), None),
        check_vma=False,
    )
```

```python
import functools
import math

import jax
import jax.numpy as jnp
from jax import lax
import numpy as np
from jax.experimental import pallas as pl
from jax.experimental.pallas import tpu as pltpu
from jax.sharding import PartitionSpec as P

BLOCK = 128
EXPERTS = 32
TOP = 2
CAP = 2
EXP_GROUP = 8


HIGHEST = lax.Precision.HIGHEST
RESIDUAL_SCALE = math.sqrt(2.0)
NORM_EPS = 1e-05
GROUP_EPS = 1e-06
ROPE_BASE = 10000.0


def entering(array, axis, join, neutral, backward):
    count = lax.axis_size(axis)
    place = lax.axis_index(axis)
    ahead = count - 1 - place if backward else place
    gathered = jax.tree.map(
        lambda a, kind: lax.all_gather(a.astype(kind), axis),
        array,
        jax.tree.map(lambda a: jnp.bfloat16 if a.dtype == jnp.float32 else a.dtype, array),
    )
    state = jax.tree.map(lambda a, e: jnp.zeros_like(a) + jnp.asarray(e, a.dtype), array, neutral)

    def one(hop, state):
        source = count - 1 - hop if backward else hop
        return join(
            state,
            jax.tree.map(
                lambda a, own: lax.dynamic_index_in_dim(a, source, 0, False).astype(own.dtype),
                gathered,
                array,
            ),
        )

    return lax.fori_loop(0, ahead, one, state)


def rotate(vectors, token_positions):
    half_width = vectors.shape[-1] // 2
    frequencies = ROPE_BASE ** (-jnp.arange(half_width, dtype=jnp.float32) / half_width)
    angles = token_positions.astype(jnp.float32)[:, None] * frequencies[None, :]
    cosine = jnp.cos(angles)[:, None, :]
    sine_part = jnp.sin(angles)[:, None, :]
    first_half = vectors[..., :half_width].astype(jnp.float32)
    second = vectors[..., half_width:].astype(jnp.float32)
    return jnp.concatenate(
        [first_half * cosine - second * sine_part, first_half * sine_part + second * cosine],
        axis=-1,
    )


def prepare(query_w, key_w, value_w, number_of_heads, token_positions):
    length = query_w.shape[0]
    queries_f = rotate(query_w.reshape(length, number_of_heads, -1), token_positions)
    key_dim = queries_f.shape[-1]
    queries = queries_f.astype(jnp.bfloat16)
    keys_rot = (
        rotate(key_w.reshape(length, number_of_heads, -1), token_positions)
        * (1.0 / math.sqrt(key_dim))
    ).astype(jnp.bfloat16)
    values = value_w.reshape(length, number_of_heads, -1)
    return (queries, keys_rot, values)


def sweep_blocks(queries, keys_rot, values, log_decay, strict, state_init, span_size):
    length, number_of_heads, key_dim = queries.shape
    value_dim = values.shape[-1]
    block_count = length // span_size

    def split_blocks(array):
        return array.reshape(block_count, span_size, number_of_heads, array.shape[-1])

    decay_blocks = log_decay.reshape(number_of_heads, block_count, span_size).transpose(1, 0, 2)
    position_index = jnp.arange(span_size)
    if strict:
        allowed = position_index[:, None] > position_index[None, :]
    else:
        allowed = position_index[:, None] >= position_index[None, :]

    def advance(state_now, inputs):
        query_blk, key_blk, value_blk, decay_blk = inputs
        cumulative = jnp.cumsum(decay_blk, axis=1)
        log_gap = cumulative[:, :, None] - cumulative[:, None, :]
        weights = jnp.where(allowed[None], jnp.exp(jnp.where(allowed[None], log_gap, 0.0)), 0.0)
        scores = (
            jnp.einsum("ihd,jhd->hij", query_blk, key_blk, preferred_element_type=jnp.float32)
            * weights
        )
        weighted = scores.astype(jnp.bfloat16)
        inner_part = jnp.einsum(
            "hij,jhv->ihv", weighted, value_blk, preferred_element_type=jnp.float32
        )
        carried = (
            jnp.einsum("ihd,hdv->ihv", query_blk.astype(jnp.float32), state_now, precision=HIGHEST)
            * jnp.exp(cumulative).T[:, :, None]
        )
        key_scaled = (
            key_blk.astype(jnp.float32) * jnp.exp(cumulative[:, -1:] - cumulative).T[:, :, None]
        )
        state_next = state_now * jnp.exp(cumulative[:, -1])[:, None, None] + jnp.einsum(
            "jhd,jhv->hdv", key_scaled, value_blk.astype(jnp.float32), precision=HIGHEST
        )
        return (state_next, inner_part + carried)

    final_state, outputs = lax.scan(
        advance,
        state_init,
        (split_blocks(queries), split_blocks(keys_rot), split_blocks(values), decay_blocks),
    )
    return (outputs.reshape(length, number_of_heads, value_dim), final_state)


def summary(keys_rot, values, log_decay):
    cumulative = jnp.cumsum(log_decay, axis=1)
    key_scaled = (
        keys_rot.astype(jnp.float32) * jnp.exp(cumulative[:, -1:] - cumulative).T[:, :, None]
    )
    return (
        jnp.exp(cumulative[:, -1]),
        jnp.einsum("lhd,lhv->hdv", key_scaled, values.astype(jnp.float32), precision=HIGHEST),
    )


def chain_states(earlier, later):
    decay_a0, state_a0, decay_b0, state_b0 = earlier
    decay_a1, state_a1, decay_b1, state_b1 = later
    return (
        decay_a0 * decay_a1,
        state_a0 * decay_a1[:, None, None] + state_a1,
        decay_b0 * decay_b1,
        state_b0 * decay_b1[:, None, None] + state_b1,
    )


def neutral(parts):
    return (
        jnp.ones_like(parts[0]),
        jnp.zeros_like(parts[1]),
        jnp.ones_like(parts[2]),
        jnp.zeros_like(parts[3]),
    )


def carry_states(forward_parts, backward_parts):
    into_forward = entering(forward_parts, "sp", chain_states, neutral(forward_parts), False)
    into_backward = entering(backward_parts, "sp", chain_states, neutral(backward_parts), True)
    return (into_forward, into_backward)


def finish(forward, backward_flipped):
    total_sum = forward + backward_flipped[::-1]
    normed = total_sum * lax.rsqrt(
        jnp.mean(total_sum * total_sum, axis=-1, keepdims=True) + GROUP_EPS
    )
    return normed.reshape(total_sum.shape[0], -1).astype(jnp.bfloat16)


def layer_norm(stream, gain):
    center = stream - jnp.mean(stream, axis=-1, keepdims=True)
    spread = jnp.mean(center * center, axis=-1, keepdims=True)
    return center * lax.rsqrt(spread + NORM_EPS) * gain


def slot_table(expert_ids):
    onehot = (expert_ids[..., None] == jnp.arange(EXPERTS, dtype=jnp.int32)).astype(jnp.int32)
    earlier = jnp.cumsum(onehot, axis=-2) - onehot
    rank_order = jnp.sum(earlier * onehot, axis=-1)
    kept_mask = rank_order < CAP
    slot_index = expert_ids * CAP + jnp.minimum(rank_order, CAP - 1)
    return (slot_index, kept_mask)


def gate_up(rows, gate_w, up_w):
    gate_part = jnp.einsum("xecd,edf->xecf", rows, gate_w, preferred_element_type=jnp.float32)
    up_part = jnp.einsum("xecd,edf->xecf", rows, up_w, preferred_element_type=jnp.float32)
    return (jax.nn.silu(gate_part) * up_part).astype(jnp.bfloat16)


def shards(
    query_a,
    key_a,
    value_a,
    decay_a,
    query_b,
    key_b,
    value_b,
    decay_b,
    out_weight_a,
    out_weight_b,
    residual,
    norm_gain,
    route_group,
    route_expert,
    route_weight,
    expert_gate,
    expert_up,
    expert_down,
):
    length = query_a.shape[0]
    token_positions = lax.axis_index("sp") * length + jnp.arange(length, dtype=jnp.int32)
    heads_a = decay_a.shape[1]
    heads_b = decay_b.shape[1]
    qa_rot, ka_rot, va_all = prepare(query_a, key_a, value_a, heads_a, token_positions)
    qb_rot, kb_rot, vb_all = prepare(query_b, key_b, value_b, heads_b, token_positions)
    flip_a = (qa_rot[::-1], ka_rot[::-1], va_all[::-1], decay_a[1][:, ::-1])
    flip_b = (qb_rot[::-1], kb_rot[::-1], vb_all[::-1], decay_b[1][:, ::-1])
    forward_parts = summary(ka_rot, va_all, decay_a[0]) + summary(kb_rot, vb_all, decay_b[0])
    backward_parts = summary(flip_a[1], flip_a[2], flip_a[3]) + summary(
        flip_b[1], flip_b[2], flip_b[3]
    )
    into_forward, into_backward = carry_states(forward_parts, backward_parts)
    forward_a = sweep_blocks(qa_rot, ka_rot, va_all, decay_a[0], False, into_forward[1], BLOCK)[0]
    forward_b = sweep_blocks(qb_rot, kb_rot, vb_all, decay_b[0], False, into_forward[3], BLOCK)[0]
    backward_a = sweep_blocks(
        flip_a[0], flip_a[1], flip_a[2], flip_a[3], True, into_backward[1], BLOCK
    )[0]
    backward_b = sweep_blocks(
        flip_b[0], flip_b[1], flip_b[2], flip_b[3], True, into_backward[3], BLOCK
    )[0]
    mixed_a = finish(forward_a, backward_a)
    mixed_b = finish(forward_b, backward_b)
    rows_dev = length // lax.axis_size("tp")
    mix = lax.psum_scatter(
        (
            jnp.dot(mixed_a, out_weight_a, preferred_element_type=jnp.float32)
            + jnp.dot(mixed_b, out_weight_b, preferred_element_type=jnp.float32)
        ).astype(jnp.bfloat16),
        "tp",
        scatter_dimension=0,
        tiled=True,
    ).astype(jnp.float32)
    hidden_in = layer_norm(
        RESIDUAL_SCALE * residual.astype(jnp.float32) + mix, norm_gain[0]
    ).astype(jnp.bfloat16)
    width = hidden_in.shape[1]
    ffn_width = expert_gate.shape[2]
    sp_count = lax.axis_size("sp")
    per_device = EXPERTS // sp_count
    slots = EXPERTS * CAP
    global_ids = (route_group[:, None] * EXP_GROUP + route_expert).reshape(-1)
    slot_index, kept_mask = slot_table(global_ids)
    hits = (slot_index[:, None] == jnp.arange(slots, dtype=jnp.int32)[None, :]) & kept_mask[:, None]
    choose = jnp.sum(hits.reshape(rows_dev, TOP, slots).astype(jnp.int32), axis=1).astype(
        jnp.bfloat16
    )
    outgoing = jnp.einsum(
        "rs,rd->sd", choose, hidden_in, preferred_element_type=jnp.float32
    ).astype(jnp.bfloat16)
    outgoing = outgoing.reshape(sp_count, per_device * CAP, width)
    received = lax.all_to_all(outgoing, "sp", split_axis=0, concat_axis=0, tiled=True)
    piece_rows = lax.all_gather(received, "tp", axis=0, tiled=True)
    piece_count = piece_rows.shape[0]
    shaped = piece_rows.reshape(-1, per_device, CAP, width)
    hidden = gate_up(shaped, expert_gate, expert_up).reshape(
        piece_count, per_device * CAP, ffn_width
    )
    flat_hidden = hidden.reshape(-1, ffn_width)
    piece_rows = flat_hidden.reshape(-1, per_device, CAP, ffn_width)
    summed = lax.psum_scatter(
        jnp.einsum("xecf,efd->xecd", piece_rows, expert_down, preferred_element_type=jnp.float32)
        .reshape(lax.axis_size("tp") * (sp_count * per_device * CAP), width)
        .astype(jnp.bfloat16),
        "tp",
        scatter_dimension=0,
        tiled=True,
    )
    back_rows = summed.reshape(sp_count, per_device * CAP, width)
    returned = lax.all_to_all(back_rows, "sp", split_axis=0, concat_axis=0, tiled=True).reshape(
        slots, width
    )
    picked = (
        jnp.take(returned, slot_index, axis=0).astype(jnp.float32).reshape(rows_dev, TOP, width)
    )
    factor = jnp.where(kept_mask.reshape(rows_dev, TOP), route_weight, 0.0)
    ffn = jnp.sum(picked * factor[..., None], axis=1)
    return layer_norm(RESIDUAL_SCALE * hidden_in.astype(jnp.float32) + ffn, norm_gain[1]).astype(
        jnp.bfloat16
    )


MESH = pl.DeviceIdType.MESH
F32 = jnp.float32
BF16 = jnp.bfloat16
NT = (((1,), (1,)), ((), ()))
TN = (((0,), (0,)), ((), ()))
LANES = 128


def dot(a, b, dims=None, precision=None):
    dims = dims or (((1,), (0,)), ((), ()))
    return lax.dot_general(a, b, dims, precision=precision, preferred_element_type=F32)


def layer_kernel(
    cfg,
    qa,
    ka,
    va,
    qb,
    kb,
    vb,
    dec_a,
    dec_b,
    cos_a,
    sin_a,
    cos_b,
    sin_b,
    start_a,
    start_b,
    head_mask,
    block_mask,
    rope_perm,
    sort_rows,
    unsort_rows,
    woa,
    wob,
    res,
    gain,
    rg,
    re,
    rw,
    eg,
    eu,
    ed,
    out,
    dec,
    wo_v,
    eg_v,
    eu_v,
    ed_v,
    qa_s,
    ka_s,
    qb_s,
    kb_s,
    acc_a,
    acc_b,
    mixed,
    loc,
    loc_b,
    dfs,
    dfs_b,
    cin,
    cin_b,
    cout,
    cout_b,
    p_out,
    p_in,
    x_out,
    x_in,
    own,
    gbuf,
    obuf,
    xs,
    hs,
    ys,
    eown,
    ep_out,
    ep_in,
    ex_out,
    ex_in,
    ret,
    fin,
    w_sem,
    wo_sem,
    c_send,
    c_recv,
    cb_send,
    cb_recv,
    p_send,
    p_recv,
    x_send,
    x_recv,
    d_send,
    g_send,
    g_recv,
    ep_send,
    ep_recv,
    ex_send,
    ex_recv,
    r_send,
    r_recv,
):
    nsp, ntp, ha, hb = cfg["nsp"], cfg["ntp"], cfg["ha"], cfg["hb"]
    half = ntp // 2
    length, width = qa.shape[0], res.shape[1]
    dka, dva = qa.shape[1] // ha, va.shape[1] // ha
    dkb = qb.shape[1] // hb
    rows = length // ntp
    cph = dva // LANES
    chunks = ha * cph
    sp, tp = lax.axis_index("sp"), lax.axis_index("tp")
    pair = tp // 2
    core = tp % 2
    mate = 2 * pair + 1 - core
    per_dev = eg.shape[0]
    tiles = p_out.shape[0]
    tile = width // tiles

    wo_copies = [
        pltpu.make_async_copy(woa, wo_v.at[pl.ds(0, ha * dva)], wo_sem.at[0]),
        pltpu.make_async_copy(wob, wo_v.at[pl.ds(ha * dva, wob.shape[0])], wo_sem.at[1]),
    ]
    for c in wo_copies:
        c.start()

    def weight_copies(e):
        return [
            pltpu.make_async_copy(a.at[e], b.at[e], w_sem.at[i, e])
            for i, (a, b) in enumerate(((eg, eg_v), (eu, eu_v), (ed, ed_v)))
        ]

    @pl.loop(0, per_dev)
    def _(e):
        for c in weight_copies(e):
            c.start()

    barrier = pltpu.get_barrier_semaphore()
    for d in range(1, nsp):
        pl.semaphore_signal(
            barrier, inc=1, device_id={"sp": (sp + d) % nsp}, device_id_type=MESH
        )
    for d in range(1, ntp):
        pl.semaphore_signal(
            barrier, inc=1, device_id={"tp": (tp + d) % ntp}, device_id_type=MESH
        )

    def remote(src, dst, ssem, rsem, axis, where):
        return pltpu.make_async_remote_copy(
            src_ref=src,
            dst_ref=dst,
            send_sem=ssem,
            recv_sem=rsem,
            device_id={axis: where},
            device_id_type=MESH,
        )

    r_i = lax.broadcasted_iota(jnp.int32, (length, length), 0)
    c_i = lax.broadcasted_iota(jnp.int32, (length, length), 1)
    lower = r_i >= c_i
    tri = jnp.where(lower, 1.0, 0.0).astype(F32)
    tri_s = jnp.where(r_i > c_i, 1.0, 0.0).astype(F32)
    for back in (0, 1):
        dec[back * ha : (back + 1) * ha] = dec_a[back]
        dec[2 * ha + back * hb : 2 * ha + (back + 1) * hb] = dec_b[back]
    d = dec[...]
    inc_col = dot(tri, d, NT, HIGHEST)
    inc_row = dot(d, tri, NT, HIGHEST)
    exc_col = dot(tri_s, d, NT, HIGHEST)
    exc_row = dot(d, tri_s, NT, HIGHEST)
    total = inc_row[:, length - 1 : length]

    def index(kind, back, h):
        return (0 if kind == "a" else 2 * ha) + (hb if kind == "b" else ha) * back + h

    def tot(kind, back, h):
        i = index(kind, back, h)
        return total[i : i + 1, :]

    def col(arr, kind, back, h):
        i = index(kind, back, h)
        return arr[:, i : i + 1]

    def row(arr, kind, back, h):
        i = index(kind, back, h)
        return arr[i : i + 1, :]

    hw = dka // 2

    def turned(start, cosine, sine):
        sc, ss = start[sp, 0:1], start[sp, 1:2]
        return sc * cosine[...] - ss * sine[...], ss * cosine[...] + sc * sine[...]

    ca, sa = turned(start_a, cos_a, sin_a)
    cb, sb = turned(start_b, cos_b, sin_b)

    def rot_a(x, scale):
        x1, x2 = x[:, :hw].astype(F32), x[:, hw:].astype(F32)
        y = jnp.concatenate([x1 * ca - x2 * sa, x1 * sa + x2 * ca], axis=1)
        return (y * scale).astype(BF16)

    masks = [head_mask[j : j + 1, :] for j in range(hb)]
    bm = block_mask[...]
    vbv = vb[...]

    def rot_b(x, scale):
        y = x.astype(F32) * cb + dot(x, rope_perm[...]) * sb
        return (y * scale).astype(BF16)

    def spread(cols):
        return functools.reduce(lambda x, y: x + y, [c * m for c, m in zip(cols, masks)])

    pl.semaphore_wait(barrier, nsp - 1 + ntp - 1)

    @pl.when(sp == 0)
    def _():
        cin[0] = jnp.zeros(cin.shape[1:], BF16)
        cin_b[0] = jnp.zeros(cin_b.shape[1:], BF16)

    @pl.when(sp == nsp - 1)
    def _():
        cin[1] = jnp.zeros(cin.shape[1:], BF16)
        cin_b[1] = jnp.zeros(cin_b.shape[1:], BF16)

    def chain_copy(back, c):
        to = (sp + nsp - 1) % nsp if back else (sp + 1) % nsp
        return remote(
            cout.at[back, c], cin.at[back, c], c_send.at[back, c], c_recv.at[back, c], "sp", to
        )

    def chain_copy_b(back):
        to = (sp + nsp - 1) % nsp if back else (sp + 1) % nsp
        return remote(
            cout_b.at[back], cin_b.at[back], cb_send.at[back], cb_recv.at[back], "sp", to
        )

    def place_of(back):
        return nsp - 1 - sp if back else sp

    def chain(back, t):
        place = place_of(back)
        c = t - 2 * (place - 1)

        @pl.when((place > 0) & (place < nsp - 1) & (c >= 0) & (c < chunks))
        def _():
            chain_copy(back, c).wait_recv()
            cout[back, c] = (
                cin[back, c].astype(F32) * dfs[back, c][:1] + loc[back, c]
            ).astype(BF16)
            chain_copy(back, c).start()

        @pl.when((place > 0) & (place < nsp - 1) & (c == chunks - 1))
        def _():
            chain_copy_b(back).wait_recv()
            cout_b[back] = (
                cin_b[back].astype(F32) * dfs_b[back][:1] + loc_b[back]
            ).astype(BF16)
            chain_copy_b(back).start()

    for h in range(ha):
        k = rot_a(ka[:, h * dka : (h + 1) * dka], 1.0 / math.sqrt(dka))
        ka_s[:, h * dka : (h + 1) * dka] = k
        kf = k.astype(F32)
        for back in (0, 1):
            if back:
                scale = jnp.exp(col(exc_col, "a", 1, h))
            else:
                scale = jnp.exp(tot("a", 0, h) - col(inc_col, "a", 0, h))
            state = dot((kf * scale).astype(BF16), va[:, h * dva : (h + 1) * dva], TN)
            for c in range(cph):
                loc[back, h * cph + c] = state[:, c * LANES : (c + 1) * LANES]
                dfs[back, h * cph + c] = jnp.broadcast_to(
                    jnp.exp(tot("a", back, h)), dfs.shape[2:]
                )

            @pl.when(place_of(back) == 0)
            def _():
                for c in range(h * cph, (h + 1) * cph):
                    cout[back, c] = loc[back, c].astype(BF16)
                    chain_copy(back, c).start()

    kbr = rot_b(kb[...], 1.0 / math.sqrt(dkb))
    kb_s[...] = kbr
    for back in (0, 1):
        if back:
            scale = spread([jnp.exp(col(exc_col, "b", 1, j)) for j in range(hb)])
        else:
            scale = spread(
                [jnp.exp(tot("b", 0, j) - col(inc_col, "b", 0, j)) for j in range(hb)]
            )
        full = dot((kbr.astype(F32) * scale).astype(BF16), vbv, TN) * bm
        loc_b[back] = functools.reduce(
            lambda x, y: x + y, [full[j * dkb : (j + 1) * dkb] for j in range(hb)]
        )
        dfs_b[back] = jnp.broadcast_to(
            spread([jnp.exp(tot("b", back, j)) for j in range(hb)]), dfs_b.shape[1:]
        )

        @pl.when(place_of(back) == 0)
        def _():
            cout_b[back] = loc_b[back].astype(BF16)
            chain_copy_b(back).start()

    def weights(kind, h):
        ahead = col(inc_col, kind, 0, h) - row(inc_row, kind, 0, h)
        behind = row(exc_row, kind, 1, h) - col(exc_col, kind, 1, h)
        return jnp.exp(jnp.minimum(jnp.where(lower, ahead, behind), 0.0))

    def local_a(h):
        q = rot_a(qa[:, h * dka : (h + 1) * dka], 1.0)
        qa_s[:, h * dka : (h + 1) * dka] = q
        s = dot(q, ka_s[:, h * dka : (h + 1) * dka], NT) * weights("a", h)
        acc_a[:, h * dva : (h + 1) * dva] = dot(
            s.astype(BF16), va[:, h * dva : (h + 1) * dva]
        )

    def local_b(j):
        if j == 0:
            qb_s[...] = rot_b(qb[...], 1.0)
        q = (qb_s[...].astype(F32) * masks[j]).astype(BF16)
        s = dot(q, kb_s[...], NT) * weights("b", j)
        part = dot(s.astype(BF16), vb[...]) * masks[j]
        if j:
            acc_b[...] += part
        else:
            acc_b[...] = part

    work = [functools.partial(local_a, h) for h in range(ha)]
    work += [functools.partial(local_b, j) for j in range(hb)]
    steps = chunks + 2 * max(nsp - 3, 0)
    work.pop(0)()
    for t in range(steps):
        chain(0, t)
        chain(1, t)
        if t < len(work):
            work[t]()
    for piece in work[steps:]:
        piece()
    for back in (0, 1):

        @pl.when(place_of(back) == nsp - 1)
        def _():
            for c in range(chunks):
                chain_copy(back, c).wait_recv()
            chain_copy_b(back).wait_recv()


    for h in range(ha):
        q = qa_s[:, h * dka : (h + 1) * dka]
        parts = []
        for back in (0, 1):
            state = jnp.concatenate([cin[back, h * cph + c] for c in range(cph)], axis=1)
            if back:
                scale = jnp.exp(tot("a", 1, h) - col(exc_col, "a", 1, h))
            else:
                scale = jnp.exp(col(inc_col, "a", 0, h))
            parts.append(dot(q, state) * scale)
        y = acc_a[:, h * dva : (h + 1) * dva] + parts[0] + parts[1]
        y = y * lax.rsqrt(jnp.mean(y * y, axis=-1, keepdims=True) + GROUP_EPS)
        mixed[:, h * dva : (h + 1) * dva] = y.astype(BF16)
    y = acc_b[...]
    for back in (0, 1):
        state = jnp.concatenate([cin_b[back].astype(F32)] * hb, axis=0) * bm
        if back:
            scale = spread([jnp.exp(tot("b", 1, j) - col(exc_col, "b", 1, j)) for j in range(hb)])
        else:
            scale = spread([jnp.exp(col(inc_col, "b", 0, j)) for j in range(hb)])
        y = y + dot(qb_s[...], state.astype(BF16)) * scale
    square = dot(y * y, bm, None, HIGHEST) * (1.0 / dkb)
    mixed[:, ha * dva :] = (y * lax.rsqrt(square + GROUP_EPS)).astype(BF16)

    for c in wo_copies:
        c.wait()

    def block(i):
        return mixed[pl.ds(pl.multiple_of(i * rows, rows), rows), :]

    theirs = jnp.concatenate([block(2 * i + 1 - core) for i in range(half)], axis=0)
    mine = jnp.concatenate([block(2 * i + core) for i in range(half)], axis=0)

    def p_copy(n):
        return remote(p_out.at[n], p_in.at[n], p_send.at[n], p_recv.at[n], "tp", mate)

    def x_copy(n, k):
        i = (pair + k) % half
        return remote(
            x_out.at[k - 1, n],
            x_in.at[k - 1, n],
            x_send.at[k - 1, n],
            x_recv.at[k - 1, n],
            "tp",
            2 * i + core,
        )

    for n in range(tiles):
        p_out[n] = dot(theirs, wo_v[:, n * tile : (n + 1) * tile]).astype(BF16)
        p_copy(n).start()
    for n in range(tiles):
        own[n] = dot(mine, wo_v[:, n * tile : (n + 1) * tile])
        p_copy(n).wait_recv()
        own[n] += p_in[n].astype(F32)
        for k in range(1, half):
            i = (pair + k) % half
            x_out[k - 1, n] = own[n, pl.ds(pl.multiple_of(i * rows, rows), rows), :].astype(BF16)
            x_copy(n, k).start()
    mix = []
    for n in range(tiles):
        m = own[n, pl.ds(pl.multiple_of(pair * rows, rows), rows), :]
        for k in range(1, half):
            x_copy(n, k).wait_recv()
            m = m + x_in[k - 1, n].astype(F32)
        mix.append(m)
    mix = jnp.concatenate(mix, axis=1)

    def norm(x, g):
        x = x - jnp.mean(x, axis=-1, keepdims=True)
        return x * lax.rsqrt(jnp.mean(x * x, axis=-1, keepdims=True) + NORM_EPS) * g

    hidden = norm(RESIDUAL_SCALE * res[...].astype(F32) + mix, gain[0:1, :]).astype(BF16)

    slots = EXPERTS * CAP
    line_e = lax.broadcasted_iota(jnp.int32, (EXPERTS, rows), 0)
    line_s = lax.broadcasted_iota(jnp.int32, (slots, rows), 0)
    ids = [rg[...] * EXP_GROUP + re[k : k + 1, :] for k in range(TOP)]
    hot = [jnp.where(i == line_e, 1.0, 0.0) for i in ids]
    before = jnp.where(
        lax.broadcasted_iota(jnp.int32, (rows, rows), 0)
        < lax.broadcasted_iota(jnp.int32, (rows, rows), 1),
        1.0,
        0.0,
    )
    earlier = dot(functools.reduce(jnp.add, hot).astype(BF16), before.astype(BF16))
    choose = []
    for i, o in zip(ids, hot):
        rank = jnp.sum(earlier * o, axis=0, keepdims=True)
        hit = jnp.zeros((slots, rows), F32)
        for c in range(CAP):
            hit = hit + jnp.where((line_s == i * CAP + c) & (rank == float(c)), 1.0, 0.0)
        choose.append(hit)
    factor = jnp.zeros((slots, rows), F32)
    for k in range(TOP):
        factor = factor + choose[k] * rw[k : k + 1, :]
    high = factor.astype(BF16)
    low = (factor - high.astype(F32)).astype(BF16)
    outgoing = dot(functools.reduce(jnp.add, choose).astype(BF16), hidden).astype(BF16)
    piece = per_dev * CAP
    for s in range(nsp):
        obuf[s] = outgoing[s * piece : (s + 1) * piece]

    def d_copy(k):
        to = (sp + k) % nsp
        return remote(
            obuf.at[to], gbuf.at[tp, sp], d_send.at[k - 1], g_recv.at[tp, sp], "sp", to
        )

    def g_copy(t, s, to, which, k):
        return remote(
            gbuf.at[t, s], gbuf.at[t, s], g_send.at[which, k], g_recv.at[t, s], "tp", to
        )

    def relay(s, k):
        for j in range(1, half):
            g_copy(tp, s, 2 * ((pair + j) % half) + core, j, k).start()
        g_copy(tp, s, mate, 0, k).start()

    order = sorted(range(1, nsp), key=lambda k: -min(k, nsp - k))
    for k in order:
        d_copy(k).start()
    gbuf[tp, sp] = obuf[sp]
    relay(sp, 0)
    for k in range(1, nsp):
        s = (sp + k) % nsp
        g_copy(tp, s, mate, 0, k).wait_recv()
        relay(s, k)
    for k in range(nsp):
        s = (sp + k) % nsp
        for j in range(1, half):
            t = 2 * ((pair + j) % half) + core
            g_copy(t, s, mate, 0, k).wait_recv()
            g_copy(t, s, mate, half + j - 1, k).start()
    for i in range(half):
        for k in range(nsp):
            g_copy(2 * i + 1 - core, (sp + k) % nsp, mate, 0, k).wait_recv()

    count = ntp * nsp * piece
    stack = count // per_dev
    xs[...] = dot(sort_rows[...], gbuf[...].reshape(count, width)).astype(BF16)

    @pl.loop(0, per_dev)
    def _(e):
        for c in weight_copies(e):
            c.wait()
        at = pl.ds(pl.multiple_of(e * stack, stack), stack)
        x = xs[at, :]
        g = dot(x, eg_v[e])
        u = dot(x, eu_v[e])
        h = (g / (1.0 + jnp.exp(-g)) * u).astype(BF16)
        hs[at, :] = h

    def ep_copy(n):
        return remote(ep_out.at[n], ep_in.at[n], ep_send.at[n], ep_recv.at[n], "tp", mate)

    def ex_copy(n, k):
        to = 2 * ((pair + k) % half) + core
        return remote(
            ex_out.at[k - 1, n],
            ex_in.at[k - 1, n],
            ex_send.at[k - 1, n],
            ex_recv.at[k - 1, n],
            "tp",
            to,
        )

    def r_copy(n, k):
        to = (sp + k) % nsp
        return remote(
            fin.at[n, to], ret.at[n, sp], r_send.at[n, k - 1], r_recv.at[n, sp], "sp", to
        )

    def r_arrival(n, k):
        s = (sp + k) % nsp
        return remote(fin.at[n, s], ret.at[n, s], r_send.at[n, k - 1], r_recv.at[n, s], "sp", s)

    group = nsp * piece
    turn = [(pair + k) % half for k in range(half)]
    to_mate = jnp.concatenate([unsort_rows[2 * i + 1 - core] for i in turn], axis=0)
    to_own = jnp.concatenate([unsort_rows[2 * i + core] for i in turn], axis=0)

    def down(n):
        for e in range(per_dev):
            y = dot(hs[e * stack : (e + 1) * stack, :], ed_v[e, :, n * tile : (n + 1) * tile])
            ys[e * stack : (e + 1) * stack, :] = y.astype(BF16)
        ep_out[n] = dot(to_mate, ys[...]).astype(BF16)
        ep_copy(n).start()
        eown[n] = dot(to_own, ys[...])

    def across(n):
        ep_copy(n).wait_recv()
        eown[n] += ep_in[n].astype(F32)
        for k in range(1, half):
            ex_out[k - 1, n] = eown[n, k * group : (k + 1) * group, :].astype(BF16)
            ex_copy(n, k).start()

    def home(n):
        z = eown[n, :group, :]
        for k in range(1, half):
            ex_copy(n, k).wait_recv()
            z = z + ex_in[k - 1, n].astype(F32)
        z = z.astype(BF16)
        for s in range(nsp):
            fin[n, s] = z[s * piece : (s + 1) * piece]
        for k in order:
            r_copy(n, k).start()
        ret[n, sp] = fin[n, sp]

    for i in range(tiles + 3):
        if i < tiles:
            down(i)
        if 0 <= i - 1 < tiles:
            across(i - 1)
        if 0 <= i - 3 < tiles:
            home(i - 3)
    ffn = []
    for n in range(tiles):
        for k in range(1, nsp):
            r_arrival(n, k).wait_recv()
        back_rows = ret[n].reshape(slots, tile)
        ffn.append(dot(high, back_rows, TN) + dot(low, back_rows, TN))
    ffn = jnp.concatenate(ffn, axis=1)
    out[...] = norm(RESIDUAL_SCALE * hidden.astype(F32) + ffn, gain[1:2, :]).astype(BF16)

    for back in (0, 1):
        place = nsp - 1 - sp if back else sp

        @pl.when(place < nsp - 1)
        def _():
            chain_copy_b(back).wait_send()
            for c in range(chunks):
                chain_copy(back, c).wait_send()

    for n in range(tiles):
        p_copy(n).wait_send()
        for k in range(1, half):
            x_copy(n, k).wait_send()
    for k in range(1, nsp):
        d_copy(k).wait_send()
        for n in range(tiles):
            r_copy(n, k).wait_send()
    for k in range(nsp):
        for which in range(2 * half - 1):
            g_copy(tp, sp, mate, which, k).wait_send()
    for n in range(tiles):
        ep_copy(n).wait_send()
        for k in range(1, half):
            ex_copy(n, k).wait_send()


def fits(mesh_sizes, heads_b, width_b, experts_here, rows):
    nsp, ntp = mesh_sizes
    aligned = (experts_here * CAP) % 16 == 0 and rows % 16 == 0 and heads_b * 64 % 128 == 0
    return ntp % 2 == 0 and ntp >= 4 and nsp >= 2 and aligned


def fused(
    query_a,
    key_a,
    value_a,
    decay_a,
    query_b,
    key_b,
    value_b,
    decay_b,
    out_weight_a,
    out_weight_b,
    residual,
    norm_gain,
    route_group,
    route_expert,
    route_weight,
    expert_gate,
    expert_up,
    expert_down,
):
    nsp, ntp = lax.axis_size("sp"), lax.axis_size("tp")
    length = query_a.shape[0]
    rows, width = residual.shape
    ha, hb = decay_a.shape[1], decay_b.shape[1]
    dka, dva = query_a.shape[1] // ha, value_a.shape[1] // ha
    dkb, wb = query_b.shape[1] // hb, query_b.shape[1]
    per_dev, _, ff = expert_gate.shape
    piece = per_dev * CAP
    half = ntp // 2
    chunks = ha * dva // LANES
    heads = 2 * (ha + hb)
    def tables(hw, copies):
        freq = ROPE_BASE ** (-np.arange(hw) / hw)
        inner = np.tile(np.arange(length)[:, None] * freq, (1, copies))
        start = np.tile((np.arange(nsp) * length)[:, None] * freq, (1, copies))
        start = np.stack([np.cos(start), np.sin(start)], axis=1)
        return [jnp.asarray(t, F32) for t in (np.cos(inner), np.sin(inner), start)]

    cos_a, sin_a, start_a = tables(dka // 2, 1)
    cos_b, sin_b, start_b = tables(dkb // 2, 2 * hb)
    lane = np.arange(wb)
    head_mask = (lane[None, :] // dkb == np.arange(hb)[:, None]).astype(np.float32)
    block_mask = (lane[None, :] // dkb == lane[:, None] // dkb).astype(np.float32)
    first = lane % dkb < dkb // 2
    perm = np.zeros((wb, wb), np.float32)
    perm[np.where(first, lane + dkb // 2, lane - dkb // 2), lane] = np.where(first, -1.0, 1.0)
    count = ntp * nsp * piece
    o = np.arange(count)
    stack = count // per_dev
    source = (o % stack) // CAP * piece + o // stack * CAP + o % CAP
    sort_rows = np.zeros((count, count), np.float32)
    sort_rows[o, source] = 1.0
    unsort_rows = sort_rows.T.reshape(ntp, nsp * piece, count)
    tiles = 4 if width % 512 == 0 else 1
    tile = width // tiles
    vmem = pl.BlockSpec(memory_space=pltpu.VMEM)
    hbm = pl.BlockSpec(memory_space=pl.ANY)
    dma = pltpu.SemaphoreType.DMA
    V = pltpu.VMEM
    return pl.pallas_call(
        functools.partial(layer_kernel, {"nsp": nsp, "ntp": ntp, "ha": ha, "hb": hb}),
        out_shape=jax.ShapeDtypeStruct((rows, width), BF16),
        in_specs=[vmem] * 19 + [hbm] * 2 + [vmem] * 5 + [hbm] * 3,
        out_specs=vmem,
        scratch_shapes=[
            V((heads, length), F32),
            V((out_weight_a.shape[0] + out_weight_b.shape[0], width), BF16),
            V(expert_gate.shape, BF16),
            V(expert_up.shape, BF16),
            V(expert_down.shape, BF16),
            V((length, ha * dka), BF16),
            V((length, ha * dka), BF16),
            V((length, wb), BF16),
            V((length, wb), BF16),
            V((length, ha * dva), F32),
            V((length, wb), F32),
            V((length, ha * dva + wb), BF16),
            V((2, chunks, dka, LANES), F32),
            V((2, dkb, wb), F32),
            V((2, chunks, 8, LANES), F32),
            V((2, 8, wb), F32),
            V((2, chunks, dka, LANES), BF16),
            V((2, dkb, wb), BF16),
            V((2, chunks, dka, LANES), BF16),
            V((2, dkb, wb), BF16),
            V((tiles, half * rows, tile), BF16),
            V((tiles, half * rows, tile), BF16),
            V((half - 1, tiles, rows, tile), BF16),
            V((half - 1, tiles, rows, tile), BF16),
            V((tiles, half * rows, tile), F32),
            V((ntp, nsp, piece, width), BF16),
            V((nsp, piece, width), BF16),
            V((count, width), BF16),
            V((count, ff), BF16),
            V((count, tile), BF16),
            V((tiles, half * nsp * piece, tile), F32),
            V((tiles, half * nsp * piece, tile), BF16),
            V((tiles, half * nsp * piece, tile), BF16),
            V((half - 1, tiles, nsp * piece, tile), BF16),
            V((half - 1, tiles, nsp * piece, tile), BF16),
            V((tiles, nsp, piece, tile), BF16),
            V((tiles, nsp, piece, tile), BF16),
            dma((3, per_dev)),
            dma((2,)),
            dma((2, chunks)),
            dma((2, chunks)),
            dma((2,)),
            dma((2,)),
            dma((tiles,)),
            dma((tiles,)),
            dma((half - 1, tiles)),
            dma((half - 1, tiles)),
            dma((nsp - 1,)),
            dma((2 * half - 1, nsp)),
            dma((ntp, nsp)),
            dma((tiles,)),
            dma((tiles,)),
            dma((half - 1, tiles)),
            dma((half - 1, tiles)),
            dma((tiles, nsp - 1)),
            dma((tiles, nsp)),
        ],
        compiler_params=pltpu.CompilerParams(
            collective_id=0, has_side_effects=True, vmem_limit_bytes=60 * 1024 * 1024
        ),
    )(
        query_a,
        key_a,
        value_a,
        query_b,
        key_b,
        value_b,
        decay_a,
        decay_b,
        cos_a,
        sin_a,
        cos_b,
        sin_b,
        start_a,
        start_b,
        jnp.asarray(head_mask),
        jnp.asarray(block_mask),
        jnp.asarray(perm, BF16),
        jnp.asarray(sort_rows, BF16),
        jnp.asarray(unsort_rows, BF16),
        out_weight_a,
        out_weight_b,
        residual,
        norm_gain,
        route_group[None, :],
        route_expert.T,
        route_weight.T,
        expert_gate,
        expert_up,
        expert_down,
    )


def layer(*args):
    sizes = (lax.axis_size("sp"), lax.axis_size("tp"))
    heads_b, experts_here, rows = args[7].shape[1], args[15].shape[0], args[10].shape[0]
    if fits(sizes, heads_b, args[4].shape[1], experts_here, rows):
        return fused(*args)
    return shards(*args)


def solution(mesh):
    return jax.shard_map(
        layer,
        mesh=mesh,
        in_specs=(
            P(("grp", "sp"), "tp"),
            P(("grp", "sp"), "tp"),
            P(("grp", "sp"), "tp"),
            P(None, "tp", ("grp", "sp")),
            P(("grp", "sp"), "tp"),
            P(("grp", "sp"), "tp"),
            P(("grp", "sp"), "tp"),
            P(None, "tp", ("grp", "sp")),
            P("tp", None),
            P("tp", None),
            P(("grp", "sp", "tp"), None),
            P(),
            P(("grp", "sp", "tp")),
            P(("grp", "sp", "tp"), None),
            P(("grp", "sp", "tp"), None),
            P("sp", None, "tp"),
            P("sp", None, "tp"),
            P("sp", "tp", None),
        ),
        out_specs=P(("grp", "sp", "tp"), None),
        check_vma=False,
    )
```
